32 devices in a mesh: ep: 16 (over z, y, x), tp: 2 (over core).
Axes of the slice: x: 2, y: 2, z: 4, core: 2. Of those that a mesh axis runs over, the one named last changes fastest.
Arguments:
- tokens: bfloat16 [512, 2048], P('ep', 'tp')
- norm1_gain: float32 [2048], P('tp'), may hold values from 0.1 to 1.9
- w_query: bfloat16 [2048, 1024], P('tp'), may hold values from -0.125 to 0.125
- w_key: bfloat16 [2048, 128], P('tp'), may hold values from -0.125 to 0.125
- w_value: bfloat16 [2048, 128], P('tp'), may hold values from -0.125 to 0.125
- head_bias: float32 [16], P('tp'), may hold values from -7 to -1.5
- key_cache: bfloat16 [512, 1024, 128], P('ep', None, 'tp'), may hold values from -6 to 6
- value_cache: bfloat16 [512, 1024, 128], P('ep', None, 'tp'), may hold values from -6 to 6
- seq_lengths: int32 [512], P('ep'), may hold values from 1 to 1024, as said below
- w_out: bfloat16 [1024, 2048], P('tp'), may hold values from -0.375 to 0.375
- norm2_gain: float32 [2048], P('tp'), may hold values from 0.5 to 8
- route_ids: int32 [512, 4], P('ep'), may hold values from 0 to 15, all different within a row; in each aligned block of 32 rows (0 to 31, 32 to 63, ...) at most 16 rows name the same one
- route_logits: float32 [512, 4], P('ep'), may hold values from -6 to 6
- expert_gate: bfloat16 [16, 2048, 2048], P('ep', None, 'tp'), may hold values from -0.125 to 0.125
- expert_up: bfloat16 [16, 2048, 2048], P('ep', None, 'tp'), may hold values from -0.125 to 0.125
- expert_down: bfloat16 [16, 2048, 2048], P('ep', 'tp'), may hold values from -0.125 to 0.125
Outputs:
- mixed_out: bfloat16 [512, 2048], P('ep', 'tp')
- new_key: bfloat16 [512, 128], P('ep', 'tp')
- new_value: bfloat16 [512, 128], P('ep', 'tp')
The draws below stay inside these ranges and needn't reach their ends.
Inputs may be any that keep to these rules, and one draw needn't show every extreme that they name: A sequence attends to its first seq_lengths cache positions; in every draw some sequence has exactly 1024. `route_ids`: each row names 4 different experts. Among the rows of one device no expert is named more than 16 times, and in every draw some expert is named exactly 16 times by some device's rows.
All inputs are finite; a program needn't handle non-finite values.
Results may differ from the reference program's by a relative error of at most 0.028.
Values may be sent and summed in bfloat16 or wider, within the bound.
A program may use at most 128 MiB of HBM per device.

```python
import math
import jax
import jax.numpy as jnp
import numpy as np
from jax import lax

D = 2048
HEAD = 64
Q_HEADS = 16
KV_HEADS = 2
FF = 2048
TOPK = 4
MAXLEN = 1024
SEQ_DEV = 32
QW = 1024
KV_W = 128
EXPERTS = 16
TOKENS = 512
CAP = 16
N_EP = 16
N_TP = 2


def draw_tokens(key, part):
    keys = jax.random.split(jax.random.fold_in(key, 11), 3)
    base = jax.random.normal(keys[0], (TOKENS, D), jnp.float32)
    ramp = 3.0 ** (jnp.arange(D, dtype=jnp.float32) / (D - 1)) / jnp.sqrt(3.0)
    rough = jnp.exp(jax.random.uniform(keys[1], (D,), jnp.float32, -0.5, 0.5))
    row_scale = jnp.exp(jax.random.uniform(keys[2], (TOKENS, 1), jnp.float32, -1.15, 1.15))
    return (base * ramp * rough * row_scale).astype(jnp.bfloat16)


def draw_seq_lengths(key, part):
    keys = jax.random.split(jax.random.fold_in(key, 23), 2)
    lengths = jax.random.randint(keys[0], (TOKENS,), 1, MAXLEN + 1, dtype=jnp.int32)
    chosen = jax.random.randint(keys[1], (), 0, TOKENS, dtype=jnp.int32)
    return jnp.where(jnp.arange(TOKENS, dtype=jnp.int32) == chosen, MAXLEN, lengths).astype(jnp.int32)


def block_levels(key, dims, shards, smallest, largest):
    loudness = 1.0
    for position, blocks in shards:
        draws = jax.random.uniform(jax.random.fold_in(jax.random.fold_in(key, 6), position), (blocks,), jnp.float32, smallest / len(shards), largest / len(shards))
        loudness = loudness * jnp.repeat(jnp.exp(draws), dims[position] // blocks).reshape((-1,) + (1,) * (len(dims) - 1 - position))
    return loudness


def deal_out(own_key, own, number, rows, number_of, top, limit, lean):
    ranking = jax.random.permutation(own_key, number_of)
    packed, usual = portions_of(number_of, rows * top, limit, lean, True), portions_of(number_of, rows * top, limit, lean, False)
    places = jnp.arange(number_of)

    def named(sizes, turn):
        used = int((sizes > 0).sum())
        fixed = max(1, used // 4)
        moved = fixed + (places - fixed + turn * (used - fixed)) % max(1, number_of - fixed)
        return jnp.zeros((number_of,), jnp.int32).at[ranking[jnp.where(places < fixed, places, moved)]].set(jnp.asarray(sizes, jnp.int32))

    sizes = jnp.where(number % 4 == 0, named(packed, number // 4), named(usual, number - number // 4 - 1))
    mixed = jax.random.permutation(jax.random.fold_in(own, 3), number_of)
    giver, taker = mixed[0:number_of // 2 * 2:2], mixed[1:number_of // 2 * 2:2]
    room = jnp.minimum(sizes[giver] - 1, limit - sizes[taker]) // 2
    room = jnp.where((giver == ranking[0]) | (taker == ranking[0]) | (sizes[taker] == 0), 0, jnp.maximum(room, 0))
    moved = jax.random.randint(jax.random.fold_in(own, 4), (number_of // 2,), 0, 1 << 20) % (room + 1)
    sizes = sizes.at[giver].add(-moved).at[taker].add(moved)
    labels = jnp.searchsorted(jnp.cumsum(sizes), jnp.arange(rows * top), side="right").astype(jnp.int32)
    grid = labels.reshape(top, rows).T
    grid = grid[jax.random.permutation(jax.random.fold_in(own, 1), rows)]
    turn = jax.random.randint(jax.random.fold_in(own, 2), (rows, 1), 0, top)
    return jnp.take_along_axis(grid, (jnp.arange(top)[None, :] + turn) % top, axis=1)


def portions_of(count, total, bound, lean, full):
    weights = [(1 << 20) // math.isqrt(standing ** lean) + 1 for standing in range(1, count + 1)]
    largest = bound if full else min(bound, max(-(-total // count), total * weights[0] // sum(weights)))
    least = 1 if total - largest >= count - 1 else 0
    holding, spare = [largest] + [least] * (count - 1), total - largest - least * (count - 1)
    while spare > 0:
        candidates = [i for i in range(1, count) if holding[i] < largest] or [i for i in range(1, count) if holding[i] < bound]
        mass, remaining = sum([weights[i] for i in candidates]), spare
        for i in candidates:
            more = min(bound - holding[i], max(1, remaining * weights[i] // mass), spare)
            holding[i] = holding[i] + more
            spare = spare - more
    return np.array(holding)


def noise(stream_key, extent, scale, reach, shards=(), kind=jnp.bfloat16):
    result = jax.random.normal(stream_key, extent, jnp.float32) * scale
    if len(shards) > 0:
        result = block_levels(stream_key, extent, shards, -0.22, 0.18) * result
    return jnp.clip(result, min=-reach, max=reach).astype(kind)


def setup_inputs(seed: int = 0) -> dict:
    seeds = jax.random.split(jax.random.key(seed), 17)
    tokens = draw_tokens(jax.random.fold_in(seeds[16], 71), 0)
    norm1_gain = jnp.clip(1.0 + 0.18 * jax.random.normal(seeds[1], (D,), jnp.float32), 0.1, 1.9)
    w_query = noise(seeds[2], (D, QW), D ** -0.5, 0.125, ((0, 2),))
    w_key = noise(seeds[3], (D, KV_W), D ** -0.5, 0.125, ((0, 2),))
    w_value = noise(seeds[4], (D, KV_W), D ** -0.5, 0.125, ((0, 2),))
    head_bias = jnp.clip(-7.0 + 5.5 * jax.random.uniform(seeds[5], (Q_HEADS,), jnp.float32) ** block_levels(seeds[5], (Q_HEADS,), ((0, 2),), -0.2, 0.2), -7.0, -1.5)
    key_cache = noise(seeds[6], (TOKENS, MAXLEN, KV_W), 1.0, 6.0, ((0, 16), (2, 2)))
    value_cache = noise(seeds[7], (TOKENS, MAXLEN, KV_W), 1.0, 6.0, ((0, 16), (2, 2)))
    seq_lengths = draw_seq_lengths(jax.random.fold_in(seeds[16], 71), 0)
    w_out = noise(seeds[9], (QW, D), (QW // 4) ** -0.5, 0.375, ((0, 2),))
    norm2_gain = jnp.clip(jnp.exp(math.log(8.0) - 2.7725887 * jax.random.uniform(seeds[10], (D,), jnp.float32) ** block_levels(seeds[10], (D,), ((0, 2),), -0.2, 0.2)), 0.5, 8.0)
    route_ids_keys = jax.random.split(jax.random.fold_in(seeds[11], 1), TOKENS // SEQ_DEV)
    route_ids_turns = jax.random.permutation(jax.random.fold_in(seeds[11], 3), TOKENS // SEQ_DEV)
    route_ids = jax.vmap(lambda own, number: deal_out(jax.random.fold_in(seeds[11], 2), own, number, SEQ_DEV, EXPERTS, TOPK, CAP, 2))(route_ids_keys, route_ids_turns).reshape((TOKENS, TOPK))
    route_logits = noise(seeds[12], (TOKENS, TOPK), 1.0, 6.0, ((0, 16),), jnp.float32)
    expert_gate = noise(seeds[13], (EXPERTS, D, FF), D ** -0.5, 0.125, ((0, 16), (2, 2)))
    expert_up = noise(seeds[14], (EXPERTS, D, FF), D ** -0.5, 0.125, ((0, 16), (2, 2)))
    expert_down = noise(seeds[15], (EXPERTS, FF, D), FF ** -0.5, 0.125, ((0, 16), (1, 2)))
    return {"tokens": tokens, "norm1_gain": norm1_gain, "w_query": w_query, "w_key": w_key, "w_value": w_value, "head_bias": head_bias, "key_cache": key_cache, "value_cache": value_cache, "seq_lengths": seq_lengths, "w_out": w_out, "norm2_gain": norm2_gain, "route_ids": route_ids, "route_logits": route_logits, "expert_gate": expert_gate, "expert_up": expert_up, "expert_down": expert_down}


LN_EPS = 1e-05
SWIGLU_ALPHA = 1.702
SWIGLU_LIMIT = 7.0

def layer_norm(values, norm_gain):
    widened = values.astype(jnp.float32)
    columns = values.shape[-1]
    average = lax.optimization_barrier(jnp.sum(widened, axis=-1, keepdims=True)) / columns
    spread = lax.optimization_barrier(jnp.sum(widened * widened, axis=-1, keepdims=True)) / columns - average * average
    return (widened - average) * lax.rsqrt(spread + LN_EPS) * norm_gain

def stick_read(query_block, key_block, value_block, length_block, head_bias):
    sequences = query_block.shape[0]
    positions = key_block.shape[1]
    kv_heads = key_block.shape[2]
    head_size = key_block.shape[3]
    grouped = query_block.reshape(sequences, kv_heads, -1, head_size)
    scores = jnp.einsum('bkgd,blkd->bkgl', grouped.astype(jnp.float32), key_block.astype(jnp.float32)) * head_size ** (-0.5)
    scores = scores + head_bias.reshape(kv_heads, -1)[None, :, :, None]
    live_mask = (lax.broadcasted_iota(jnp.int32, (sequences, positions), 1) < length_block[:, None])[:, None, None, :]
    spent_log = jnp.where(live_mask, jax.nn.softplus(scores), 0.0)
    tail_sum = lax.cumsum(spent_log, axis=3, reverse=True) - spent_log
    weights = jnp.where(live_mask, jnp.exp(jax.nn.log_sigmoid(scores) - tail_sum), 0.0).astype(jnp.bfloat16)
    mixture = jnp.einsum('bkgl,blkd->bkgd', weights.astype(jnp.float32), value_block.astype(jnp.float32))
    return mixture.astype(jnp.bfloat16).reshape(sequences, -1)

def expert_rows(rows_in, gate_weight, up_weight, down_weight):
    gate_pre = jnp.dot(rows_in, gate_weight, preferred_element_type=jnp.float32)
    up_pre = jnp.dot(rows_in, up_weight, preferred_element_type=jnp.float32)
    clipped = jnp.minimum(gate_pre, SWIGLU_LIMIT)
    linear = jnp.clip(up_pre, -SWIGLU_LIMIT, SWIGLU_LIMIT)
    activated = (clipped * jax.nn.sigmoid(SWIGLU_ALPHA * clipped) * (linear + 1.0)).astype(jnp.bfloat16)
    hidden_cols = FF // N_TP
    running = jnp.zeros((rows_in.shape[0], D), jnp.float32)
    for portion in range(N_TP):
        partial_value = jnp.dot(activated[:, portion * hidden_cols:(portion + 1) * hidden_cols], down_weight[portion * hidden_cols:(portion + 1) * hidden_cols], preferred_element_type=jnp.float32)
        running = running + lax.optimization_barrier(partial_value.astype(jnp.bfloat16)).astype(jnp.float32)
    return running.astype(jnp.bfloat16)

def slots_of(ids_block):
    flat_ids = ids_block.reshape(-1)
    expert_hot = (flat_ids[:, None] == jnp.arange(EXPERTS, dtype=jnp.int32)[None, :]).astype(jnp.int32)
    earlier = jnp.cumsum(expert_hot, axis=0, dtype=jnp.int32) - expert_hot
    return flat_ids * CAP + lax.optimization_barrier(jnp.sum(earlier * expert_hot, axis=1, dtype=jnp.int32))

def reference(tokens, norm1_gain, w_query, w_key, w_value, head_bias, key_cache, value_cache, seq_lengths, w_out, norm2_gain, route_ids, route_logits, expert_gate, expert_up, expert_down):
    normed = layer_norm(tokens, norm1_gain).astype(jnp.bfloat16)
    query_rows = jnp.dot(normed, w_query, preferred_element_type=jnp.float32).astype(jnp.bfloat16)
    new_key = jnp.dot(normed, w_key, preferred_element_type=jnp.float32).astype(jnp.bfloat16)
    new_value = jnp.dot(normed, w_value, preferred_element_type=jnp.float32).astype(jnp.bfloat16)

    def read_block(items):
        return stick_read(items[0], items[1], items[2], items[3], head_bias)
    attended = lax.map(read_block, (query_rows.reshape(N_EP, SEQ_DEV, QW), key_cache.reshape(N_EP, SEQ_DEV, MAXLEN, KV_HEADS, HEAD), value_cache.reshape(N_EP, SEQ_DEV, MAXLEN, KV_HEADS, HEAD), seq_lengths.reshape(N_EP, SEQ_DEV)))
    attended = attended.reshape(TOKENS, QW)
    head_cols = QW // N_TP
    branch = jnp.zeros((TOKENS, D), jnp.float32)
    for portion in range(N_TP):
        partial_value = jnp.dot(attended[:, portion * head_cols:(portion + 1) * head_cols], w_out[portion * head_cols:(portion + 1) * head_cols], preferred_element_type=jnp.float32)
        branch = branch + lax.optimization_barrier(partial_value.astype(jnp.bfloat16)).astype(jnp.float32)
    residual = (tokens.astype(jnp.float32) + branch).astype(jnp.bfloat16)
    normed_two = layer_norm(residual, norm2_gain).astype(jnp.bfloat16)
    targets = jax.vmap(slots_of)(route_ids.reshape(N_EP, SEQ_DEV, TOPK))
    sources = jnp.repeat(normed_two.reshape(N_EP, SEQ_DEV, D), TOPK, axis=1)
    device_ids = jnp.arange(N_EP, dtype=jnp.int32)[:, None]
    dispatch = jnp.zeros((N_EP, EXPERTS * CAP, D), jnp.bfloat16).at[device_ids, targets].set(sources)
    by_expert = dispatch.reshape(N_EP, EXPERTS, CAP, D).transpose(1, 0, 2, 3).reshape(EXPERTS, N_EP * CAP, D)

    def run_one(items):
        return expert_rows(items[0], items[1], items[2], items[3])
    results = lax.map(run_one, (by_expert, expert_gate, expert_up, expert_down))
    by_source = results.reshape(EXPERTS, N_EP, CAP, D).transpose(1, 0, 2, 3).reshape(N_EP, EXPERTS * CAP, D)
    picked = by_source[device_ids, targets].reshape(TOKENS, TOPK, D).astype(jnp.float32)
    exp_logits = jnp.exp(route_logits)
    route_probs = exp_logits / lax.optimization_barrier(jnp.sum(exp_logits, axis=1, keepdims=True))
    moe_out = lax.optimization_barrier(jnp.sum(route_probs[:, :, None] * picked, axis=1))
    mixed_out = (residual.astype(jnp.float32) + moe_out).astype(jnp.bfloat16)
    return (mixed_out, new_key, new_value)
```

```python
import functools

import jax
import jax.numpy as jnp
from jax import lax
from jax.experimental import pallas as pl
from jax.experimental.pallas import tpu as pltpu
from jax.sharding import PartitionSpec as P

HEAD = 64
LN_EPS = 1e-05
SWIGLU_ALPHA = 1.702
SWIGLU_LIMIT = 7.0
MESH = pl.DeviceIdType.MESH
F32 = jnp.float32
BF16 = jnp.bfloat16
DEAD = -1e30
POS_BLOCK = 256
COL_BLOCK = 256


def dot(a, b):
    return jnp.dot(a, b, preferred_element_type=F32)


def kernel(
    n,
    cap,
    tok_hbm,
    g1_hbm,
    wq_hbm,
    wk_hbm,
    wv_hbm,
    bias_ref,
    kc_hbm,
    vc_hbm,
    lens_ref,
    wo_hbm,
    g2_hbm,
    ids_hbm,
    logits_hbm,
    gate_hbm,
    up_hbm,
    down_hbm,
    out_ref,
    nk_ref,
    nv_ref,
    x_own,
    x_peer,
    g1,
    wq,
    wk,
    wv,
    kc,
    vc,
    wo,
    g2,
    ids,
    logits,
    gate,
    up,
    down,
    proj_send,
    proj_recv,
    q_rows,
    z_ref,
    att_ref,
    part_send,
    part_recv,
    res_ref,
    disp,
    recv_own,
    recv_peer,
    gate_acc,
    up_acc,
    act_ref,
    down_send,
    down_recv,
    down_own,
    back_send,
    back_recv,
    comb_ref,
    load_sem,
    one_send,
    one_recv,
    disp_send_sem,
    disp_recv_sem,
    fwd_send_sem,
    fwd_recv_sem,
    down_send_sem,
    down_recv_sem,
    back_send_sem,
    back_recv_sem,
    local_sem,
):
    ep = lax.axis_index("ep")
    tp = lax.axis_index("tp")
    other = 1 - tp
    seqs, half = x_own.shape
    width = 2 * half
    slots = n * cap

    loads = []
    pairs = (
        (tok_hbm, x_own),
        (g1_hbm, g1),
        (wq_hbm, wq),
        (wk_hbm, wk),
        (wv_hbm, wv),
        (kc_hbm, kc),
        (vc_hbm, vc),
        (wo_hbm, wo),
        (g2_hbm, g2),
        (ids_hbm, ids),
        (logits_hbm, logits),
        (gate_hbm, gate),
        (up_hbm, up),
        (down_hbm, down),
    )
    for i, (src, dst) in enumerate(pairs):
        copy = pltpu.make_async_copy(src, dst, load_sem.at[i])
        copy.start()
        loads.append(copy)

    def peer_copy(src, dst, i):
        return pltpu.make_async_remote_copy(
            src_ref=src,
            dst_ref=dst,
            send_sem=one_send.at[i],
            recv_sem=one_recv.at[i],
            device_id=(ep, other),
            device_id_type=MESH,
        )

    barrier = pltpu.get_barrier_semaphore()
    pl.semaphore_signal(barrier, inc=1, device_id=(ep, other), device_id_type=MESH)

    def greet(i, carry):
        pl.semaphore_signal(
            barrier, inc=1, device_id=(lax.rem(ep + i, n), tp), device_id_type=MESH
        )
        return carry

    lax.fori_loop(1, n, greet, 0)
    pl.semaphore_wait(barrier, n)

    loads[0].wait()
    tok_copy = peer_copy(x_own, x_peer, 0)
    tok_copy.start()
    loads[1].wait()
    for i in (2, 3, 4):
        loads[i].wait()
    mine = x_own[...].astype(F32)
    tok_copy.wait()
    theirs = x_peer[...].astype(F32)

    def stats(a, b):
        total = jnp.sum(a, axis=1, keepdims=True) + jnp.sum(b, axis=1, keepdims=True)
        square = jnp.sum(a * a, axis=1, keepdims=True) + jnp.sum(b * b, axis=1, keepdims=True)
        mean = total / width
        return mean, lax.rsqrt(square / width - mean * mean + LN_EPS)

    mean, scale = stats(mine, theirs)
    normed = ((mine - mean) * scale * g1[...]).astype(BF16)
    pq = dot(normed, wq[...])
    pk = dot(normed, wk[...])
    pv = dot(normed, wv[...])
    qc = pq.shape[1] // 2
    kcols = pk.shape[1] // 2
    first = tp == 0
    proj_send[:, :qc] = jnp.where(first, pq[:, qc:], pq[:, :qc])
    proj_send[:, qc : qc + kcols] = jnp.where(first, pk[:, kcols:], pk[:, :kcols])
    proj_send[:, qc + kcols :] = jnp.where(first, pv[:, kcols:], pv[:, :kcols])
    proj_copy = peer_copy(proj_send, proj_recv, 1)
    proj_copy.start()

    loads[9].wait()
    loads[10].wait()
    top = ids.shape[0]
    slot_row = lax.broadcasted_iota(jnp.int32, (slots, seqs), 0)
    slot_expert = slot_row // cap
    slot_rank = slot_row - slot_expert * cap
    id_rows = ids[...]
    raw = jnp.exp(logits[...])
    probs = raw / jnp.sum(raw, axis=0, keepdims=True)
    hot = jnp.zeros((slots, seqs), F32)
    prob_hot = jnp.zeros((slots, seqs), F32)
    for k in range(top):
        match = id_rows[k : k + 1, :] == slot_expert
        hot = hot + jnp.where(match, 1.0, 0.0)
        prob_hot = prob_hot + jnp.where(match, probs[k : k + 1, :], 0.0)
    earlier = (
        lax.broadcasted_iota(jnp.int32, (seqs, seqs), 0)
        < lax.broadcasted_iota(jnp.int32, (seqs, seqs), 1)
    )
    rank = dot(hot.astype(BF16), jnp.where(earlier, 1.0, 0.0).astype(BF16))
    chosen = (hot > 0.5) & (jnp.abs(rank - slot_rank.astype(F32)) < 0.5)
    placing = jnp.where(chosen, 1.0, 0.0).astype(BF16)
    weight = jnp.where(chosen, prob_hot, 0.0)
    weight_hi = weight.astype(BF16)
    weight_lo = (weight - weight_hi.astype(F32)).astype(BF16)
    comb_ref[0] = weight_hi
    comb_ref[1] = weight_lo

    groups = qc // HEAD
    bias = jnp.zeros((groups, 1), F32)
    head_row = lax.broadcasted_iota(jnp.int32, (groups, 1), 0)
    for h in range(groups):
        bias = bias + jnp.where(head_row == h, bias_ref[h], 0.0)

    own_q = jnp.where(first, pq[:, :qc], pq[:, qc:])
    own_k = jnp.where(first, pk[:, :kcols], pk[:, kcols:])
    own_v = jnp.where(first, pv[:, :kcols], pv[:, kcols:])
    proj_copy.wait()
    query = (own_q + proj_recv[:, :qc]).astype(BF16).astype(F32)
    nk_ref[...] = (own_k + proj_recv[:, qc : qc + kcols]).astype(BF16)
    nv_ref[...] = (own_v + proj_recv[:, qc + kcols :]).astype(BF16)
    for h in range(groups):
        q_rows[:, h, :] = query[:, h * HEAD : (h + 1) * HEAD]

    positions = kc.shape[2]
    loads[5].wait()
    place = lax.broadcasted_iota(jnp.int32, (groups, positions), 1)

    def score_step(i, carry):
        for j in range(4):
            b = i * 4 + j
            s = dot(q_rows[b].astype(BF16), kc[b]) * HEAD ** (-0.5) + bias
            z_ref[pl.ds(pl.multiple_of(b * groups, groups), groups), :] = jnp.where(
                place < lens_ref[b], s, DEAD
            )
        return carry

    lax.fori_loop(0, seqs // 4, score_step, 0)

    after = (
        lax.broadcasted_iota(jnp.int32, (POS_BLOCK, POS_BLOCK), 0)
        > lax.broadcasted_iota(jnp.int32, (POS_BLOCK, POS_BLOCK), 1)
    )
    after = jnp.where(after, 1.0, 0.0).astype(BF16)
    row_block = 64

    def break_step(i, carry):
        rows = pl.ds(pl.multiple_of(i * row_block, row_block), row_block)
        beyond = jnp.zeros((row_block, 1), F32)
        for c in reversed(range(positions // POS_BLOCK)):
            cols = slice(c * POS_BLOCK, (c + 1) * POS_BLOCK)
            z = z_ref[rows, cols]
            tail = jnp.log1p(jnp.exp(-jnp.abs(z)))
            spent = jnp.maximum(z, 0.0) + tail
            hi = spent.astype(BF16)
            lo = (spent - hi.astype(F32)).astype(BF16)
            sums = dot(jnp.concatenate([hi, lo], axis=0), after)
            inside = sums[:row_block] + sums[row_block:]
            z_ref[rows, cols] = jnp.exp(jnp.minimum(z, 0.0) - tail - (inside + beyond))
            beyond = beyond + inside[:, :1] + spent[:, :1]
        return carry

    lax.fori_loop(0, seqs * groups // row_block, break_step, 0)

    loads[6].wait()

    def read_step(i, carry):
        rows = pl.ds(pl.multiple_of(i * 4 * groups, 4 * groups), 4 * groups)
        weights = z_ref[rows, :].astype(BF16)
        values = vc[pl.ds(i * 4, 4)].reshape(4 * HEAD, positions)
        mixed = lax.dot_general(
            weights, values, (((1,), (1,)), ((), ())), preferred_element_type=F32
        )
        for j in range(4):
            att_ref[i * 4 + j] = mixed[
                j * groups : (j + 1) * groups, j * HEAD : (j + 1) * HEAD
            ]
        return carry

    lax.fori_loop(0, seqs // 4, read_step, 0)
    attended = jnp.concatenate([att_ref[:, h, :] for h in range(groups)], axis=1).astype(BF16)

    loads[7].wait()
    part = dot(attended, wo[...]).astype(BF16)
    part_send[0] = part[:, :half]
    part_send[1] = part[:, half:]
    part_copy = peer_copy(part_send, part_recv, 2)
    part_copy.start()
    loads[8].wait()
    part_copy.wait()
    mine = x_own[...].astype(F32)
    theirs = x_peer[...].astype(F32)
    res_own = (mine + (part_send[tp].astype(F32) + part_recv[tp].astype(F32))).astype(BF16)
    res_other = (
        theirs + (part_send[other].astype(F32) + part_recv[other].astype(F32))
    ).astype(BF16)
    res_ref[...] = res_own
    mine = res_own.astype(F32)
    mean, scale = stats(mine, res_other.astype(F32))
    normed_two = ((mine - mean) * scale * g2[...]).astype(BF16)
    disp[...] = dot(placing, normed_two).astype(BF16).reshape(n, cap, half)

    def disp_copy(i):
        to = lax.rem(ep + i, n)
        return pltpu.make_async_remote_copy(
            src_ref=disp.at[to],
            dst_ref=recv_own.at[ep],
            send_sem=disp_send_sem.at[i],
            recv_sem=disp_recv_sem.at[i],
            device_id=(to, tp),
            device_id_type=MESH,
        )

    def disp_arrival(i):
        source = lax.rem(ep + n - i, n)
        return pltpu.make_async_remote_copy(
            src_ref=disp.at[source],
            dst_ref=recv_own.at[source],
            send_sem=disp_send_sem.at[i],
            recv_sem=disp_recv_sem.at[i],
            device_id=(source, tp),
            device_id_type=MESH,
        )

    def fwd_copy(i):
        source = lax.rem(ep + n - i, n)
        return pltpu.make_async_remote_copy(
            src_ref=recv_own.at[source],
            dst_ref=recv_peer.at[source],
            send_sem=fwd_send_sem.at[i],
            recv_sem=fwd_recv_sem.at[i],
            device_id=(ep, other),
            device_id_type=MESH,
        )

    def start_disp(i, carry):
        disp_copy(i).start()
        return carry

    lax.fori_loop(1, n, start_disp, 0)
    keep = pltpu.make_async_copy(disp.at[ep], recv_own.at[ep], local_sem.at[0])
    keep.start()
    keep.wait()
    fwd_copy(0).start()

    def pass_on(i, carry):
        disp_arrival(i).wait_recv()
        fwd_copy(i).start()
        return carry

    lax.fori_loop(1, n, pass_on, 0)

    loads[11].wait()
    loads[12].wait()
    rows_block = min(slots, 256)
    row_blocks = slots // rows_block
    per_block = rows_block // cap
    hidden = gate.shape[1]

    def first_half(i, carry):
        cols = pl.ds(pl.multiple_of(i * COL_BLOCK, COL_BLOCK), COL_BLOCK)
        depth = pl.ds(pl.multiple_of(tp * half, half), half)
        for r in range(row_blocks):
            rows = recv_own[r * per_block : (r + 1) * per_block].reshape(rows_block, half)
            at = slice(r * rows_block, (r + 1) * rows_block)
            gate_acc[at, cols] = dot(rows, gate[depth, cols])
            up_acc[at, cols] = dot(rows, up[depth, cols])
        return carry

    lax.fori_loop(0, hidden // COL_BLOCK, first_half, 0)

    def finish_fwd(i, carry):
        fwd_copy(i).wait()
        return carry

    lax.fori_loop(0, n, finish_fwd, 0)

    def second_half(i, carry):
        cols = pl.ds(pl.multiple_of(i * COL_BLOCK, COL_BLOCK), COL_BLOCK)
        depth = pl.ds(pl.multiple_of(other * half, half), half)
        for r in range(row_blocks):
            rows = recv_peer[r * per_block : (r + 1) * per_block].reshape(rows_block, half)
            at = slice(r * rows_block, (r + 1) * rows_block)
            g = gate_acc[at, cols] + dot(rows, gate[depth, cols])
            u = up_acc[at, cols] + dot(rows, up[depth, cols])
            c = jnp.minimum(g, SWIGLU_LIMIT)
            linear = jnp.clip(u, -SWIGLU_LIMIT, SWIGLU_LIMIT)
            act_ref[at, cols] = (
                c * jax.nn.sigmoid(SWIGLU_ALPHA * c) * (linear + 1.0)
            ).astype(BF16)
        return carry

    lax.fori_loop(0, hidden // COL_BLOCK, second_half, 0)

    loads[13].wait()
    tiles = half // COL_BLOCK

    def down_copy(i):
        return pltpu.make_async_remote_copy(
            src_ref=down_send.at[i],
            dst_ref=down_recv.at[i],
            send_sem=down_send_sem.at[i],
            recv_sem=down_recv_sem.at[i],
            device_id=(ep, other),
            device_id_type=MESH,
        )

    def down_tile(ref, side, i):
        cols = pl.ds(pl.multiple_of(side * half + i * COL_BLOCK, COL_BLOCK), COL_BLOCK)
        for r in range(row_blocks):
            at = slice(r * rows_block, (r + 1) * rows_block)
            ref[i, at, :] = dot(act_ref[at, :], down[:, cols]).astype(BF16)

    def down_other(i, carry):
        down_tile(down_send, other, i)
        down_copy(i).start()
        return carry

    lax.fori_loop(0, tiles, down_other, 0)

    def down_mine(i, carry):
        down_tile(down_own, tp, i)
        return carry

    lax.fori_loop(0, tiles, down_mine, 0)
    for i in range(tiles):
        down_copy(i).wait()
        total = (down_own[i].astype(F32) + down_recv[i].astype(F32)).astype(BF16)
        back_send[:, :, i * COL_BLOCK : (i + 1) * COL_BLOCK] = total.reshape(n, cap, COL_BLOCK)

    def back_copy(i):
        to = lax.rem(ep + i, n)
        return pltpu.make_async_remote_copy(
            src_ref=back_send.at[to],
            dst_ref=back_recv.at[ep],
            send_sem=back_send_sem.at[i],
            recv_sem=back_recv_sem.at[i],
            device_id=(to, tp),
            device_id_type=MESH,
        )

    def back_arrival(i):
        source = lax.rem(ep + n - i, n)
        return pltpu.make_async_remote_copy(
            src_ref=back_send.at[source],
            dst_ref=back_recv.at[source],
            send_sem=back_send_sem.at[i],
            recv_sem=back_recv_sem.at[i],
            device_id=(source, tp),
            device_id_type=MESH,
        )

    def start_back(i, carry):
        back_copy(i).start()
        return carry

    lax.fori_loop(1, n, start_back, 0)
    keep = pltpu.make_async_copy(back_send.at[ep], back_recv.at[ep], local_sem.at[1])
    keep.start()
    keep.wait()

    def finish_back(i, carry):
        back_arrival(i).wait_recv()
        return carry

    lax.fori_loop(1, n, finish_back, 0)

    back = back_recv[...].reshape(slots, half)
    over_slots = (((0,), (0,)), ((), ()))
    moe = lax.dot_general(comb_ref[0], back, over_slots, preferred_element_type=F32)
    moe = moe + lax.dot_general(comb_ref[1], back, over_slots, preferred_element_type=F32)
    out_ref[...] = (res_ref[...].astype(F32) + moe).astype(BF16)

    def finish_sends(i, carry):
        disp_copy(i).wait_send()
        back_copy(i).wait_send()
        return carry

    lax.fori_loop(1, n, finish_sends, 0)


def local(
    tokens,
    norm1_gain,
    w_query,
    w_key,
    w_value,
    head_bias,
    key_cache,
    value_cache,
    seq_lengths,
    w_out,
    norm2_gain,
    route_ids,
    route_logits,
    expert_gate,
    expert_up,
    expert_down,
):
    n = lax.axis_size("ep")
    seqs, half = tokens.shape
    top = route_ids.shape[1]
    experts = n * expert_gate.shape[0]
    capacity = max(2, 2 * seqs * top // experts)
    cap = -(-capacity // 16) * 16
    slots = n * cap
    qc = w_query.shape[1] // 2
    kcols = w_key.shape[1] // 2
    groups = qc // HEAD
    positions = key_cache.shape[1]
    hidden = expert_gate.shape[2]
    tiles = half // COL_BLOCK
    keys = jnp.swapaxes(key_cache, 1, 2)
    values = jnp.swapaxes(value_cache, 1, 2)
    operands = (
        tokens,
        norm1_gain.reshape(1, -1),
        w_query,
        w_key,
        w_value,
        head_bias,
        keys,
        values,
        seq_lengths,
        w_out,
        norm2_gain.reshape(1, -1),
        route_ids.T,
        route_logits.T,
        expert_gate.reshape(expert_gate.shape[1:]),
        expert_up.reshape(expert_up.shape[1:]),
        expert_down.reshape(expert_down.shape[1:]),
    )
    in_smem = (5, 8)
    in_specs = [
        pl.BlockSpec(memory_space=pltpu.SMEM if i in in_smem else pl.ANY)
        for i in range(len(operands))
    ]
    vmem = pl.BlockSpec(memory_space=pltpu.VMEM)
    loaded = [
        pltpu.VMEM(a.shape, a.dtype) for i, a in enumerate(operands) if i not in in_smem
    ]
    dma = pltpu.SemaphoreType.DMA
    scratch = (
        [loaded[0], loaded[0]]
        + loaded[1:]
        + [
            pltpu.VMEM((seqs, qc + 2 * kcols), F32),
            pltpu.VMEM((seqs, qc + 2 * kcols), F32),
            pltpu.VMEM((seqs, groups, HEAD), F32),
            pltpu.VMEM((seqs * groups, positions), F32),
            pltpu.VMEM((seqs, groups, HEAD), F32),
            pltpu.VMEM((2, seqs, half), BF16),
            pltpu.VMEM((2, seqs, half), BF16),
            pltpu.VMEM((seqs, half), BF16),
            pltpu.VMEM((n, cap, half), BF16),
            pltpu.VMEM((n, cap, half), BF16),
            pltpu.VMEM((n, cap, half), BF16),
            pltpu.VMEM((slots, hidden), F32),
            pltpu.VMEM((slots, hidden), F32),
            pltpu.VMEM((slots, hidden), BF16),
            pltpu.VMEM((tiles, slots, COL_BLOCK), BF16),
            pltpu.VMEM((tiles, slots, COL_BLOCK), BF16),
            pltpu.VMEM((tiles, slots, COL_BLOCK), BF16),
            pltpu.VMEM((n, cap, half), BF16),
            pltpu.VMEM((n, cap, half), BF16),
            pltpu.VMEM((2, slots, seqs), BF16),
            dma((len(loaded),)),
            dma((3,)),
            dma((3,)),
            dma((n,)),
            dma((n,)),
            dma((n,)),
            dma((n,)),
            dma((tiles,)),
            dma((tiles,)),
            dma((n,)),
            dma((n,)),
            dma((2,)),
        ]
    )
    return pl.pallas_call(
        functools.partial(kernel, n, cap),
        out_shape=(
            jax.ShapeDtypeStruct((seqs, half), BF16),
            jax.ShapeDtypeStruct((seqs, kcols), BF16),
            jax.ShapeDtypeStruct((seqs, kcols), BF16),
        ),
        in_specs=in_specs,
        out_specs=(vmem, vmem, vmem),
        scratch_shapes=scratch,
        compiler_params=pltpu.CompilerParams(
            collective_id=0, has_side_effects=True, vmem_limit_bytes=64 * 1024 * 1024 - 65536
        ),
    )(*operands)


def solution(mesh):
    in_specs = (
        P("ep", "tp"),
        P("tp"),
        P("tp", None),
        P("tp", None),
        P("tp", None),
        P("tp"),
        P("ep", None, "tp"),
        P("ep", None, "tp"),
        P("ep"),
        P("tp", None),
        P("tp"),
        P("ep", None),
        P("ep", None),
        P("ep", None, "tp"),
        P("ep", None, "tp"),
        P("ep", "tp", None),
    )
    out_specs = (P("ep", "tp"), P("ep", "tp"), P("ep", "tp"))
    return jax.shard_map(local, mesh=mesh, in_specs=in_specs, out_specs=out_specs, check_vma=False)
```

```python
import functools

import jax
import jax.numpy as jnp
from jax import lax
from jax.experimental import pallas as pl
from jax.experimental.pallas import tpu as pltpu
from jax.sharding import PartitionSpec as P

HEAD = 64
LN_EPS = 1e-05
SWIGLU_ALPHA = 1.702
SWIGLU_LIMIT = 7.0
MESH = pl.DeviceIdType.MESH
F32 = jnp.float32
BF16 = jnp.bfloat16
DEAD = -1e30
POS_BLOCK = 256
COL_BLOCK = 256


def dot(a, b):
    return jnp.dot(a, b, preferred_element_type=F32)


def kernel(
    n,
    cap,
    tok_hbm,
    g1_hbm,
    wq_hbm,
    wk_hbm,
    wv_hbm,
    bias_ref,
    kc_hbm,
    vc_hbm,
    lens_ref,
    wo_hbm,
    g2_hbm,
    ids_hbm,
    logits_hbm,
    gate_hbm,
    up_hbm,
    down_hbm,
    out_ref,
    nk_ref,
    nv_ref,
    x_own,
    x_peer,
    g1,
    wq,
    wk,
    wv,
    kc,
    vc,
    wo,
    g2,
    ids,
    logits,
    gate,
    up,
    down,
    proj_send,
    proj_recv,
    q_rows,
    z_ref,
    att_ref,
    part_send,
    part_recv,
    res_ref,
    tables_send,
    tables_recv,
    rows_ref,
    rows_recv,
    disp,
    recv_own,
    recv_peer,
    gate_acc,
    up_acc,
    act_ref,
    down_send,
    down_recv,
    down_own,
    back_send,
    back_recv,
    sum_send,
    sum_recv,
    load_sem,
    one_send,
    one_recv,
    table_send_sem,
    table_recv_sem,
    rows_send_sem,
    rows_recv_sem,
    sum_send_sem,
    sum_recv_sem,
    disp_send_sem,
    disp_recv_sem,
    fwd_send_sem,
    fwd_recv_sem,
    down_send_sem,
    down_recv_sem,
    back_send_sem,
    back_recv_sem,
    local_sem,
):
    ep = lax.axis_index("ep")
    tp = lax.axis_index("tp")
    other = 1 - tp
    seqs, half = x_own.shape
    width = 2 * half
    slots = n * cap

    loads = []
    pairs = (
        (tok_hbm, x_own),
        (g1_hbm, g1),
        (wq_hbm, wq),
        (wk_hbm, wk),
        (wv_hbm, wv),
        (kc_hbm, kc),
        (vc_hbm, vc),
        (wo_hbm, wo),
        (g2_hbm, g2),
        (ids_hbm, ids),
        (logits_hbm, logits),
        (gate_hbm, gate),
        (up_hbm, up),
        (down_hbm, down),
    )
    for i, (src, dst) in enumerate(pairs):
        copy = pltpu.make_async_copy(src, dst, load_sem.at[i])
        loads.append(copy)
    for i in (0, 2, 3, 4, 1, 9, 10, 8):
        loads[i].start()

    def peer_copy(src, dst, i):
        return pltpu.make_async_remote_copy(
            src_ref=src,
            dst_ref=dst,
            send_sem=one_send.at[i],
            recv_sem=one_recv.at[i],
            device_id=(ep, other),
            device_id_type=MESH,
        )

    barrier = pltpu.get_barrier_semaphore()
    pl.semaphore_signal(barrier, inc=1, device_id=(ep, other), device_id_type=MESH)

    planes = tables_send.shape[0]
    plane = n // planes
    level = ep // plane
    spot = ep % plane

    def column(i):
        return lax.rem(level + i, planes) * plane + spot

    def beside(i):
        return level * plane + lax.rem(spot + i, plane)

    def greet_column(i, carry):
        pl.semaphore_signal(barrier, inc=1, device_id=(column(i), tp), device_id_type=MESH)
        return carry

    def greet_beside(i, carry):
        pl.semaphore_signal(barrier, inc=1, device_id=(beside(i), tp), device_id_type=MESH)
        return carry

    lax.fori_loop(1, planes, greet_column, 0)
    lax.fori_loop(1, plane, greet_beside, 0)
    pl.semaphore_wait(barrier, planes + plane - 1)

    loads[0].wait()
    tok_copy = peer_copy(x_own, x_peer, 0)
    tok_copy.start()
    loads[1].wait()
    for i in (2, 3, 4):
        loads[i].wait()
    for i in (5, 6, 7):
        loads[i].start()
    mine = x_own[...].astype(F32)
    tok_copy.wait()
    theirs = x_peer[...].astype(F32)

    def stats(a, b):
        total = jnp.sum(a, axis=1, keepdims=True) + jnp.sum(b, axis=1, keepdims=True)
        square = jnp.sum(a * a, axis=1, keepdims=True) + jnp.sum(b * b, axis=1, keepdims=True)
        mean = total / width
        return mean, lax.rsqrt(square / width - mean * mean + LN_EPS)

    mean, scale = stats(mine, theirs)
    normed = ((mine - mean) * scale * g1[...]).astype(BF16)
    pq = dot(normed, wq[...])
    pk = dot(normed, wk[...])
    pv = dot(normed, wv[...])
    qc = pq.shape[1] // 2
    kcols = pk.shape[1] // 2
    first = tp == 0
    proj_send[:, :qc] = jnp.where(first, pq[:, qc:], pq[:, :qc])
    proj_send[:, qc : qc + kcols] = jnp.where(first, pk[:, kcols:], pk[:, :kcols])
    proj_send[:, qc + kcols :] = jnp.where(first, pv[:, kcols:], pv[:, :kcols])
    proj_copy = peer_copy(proj_send, proj_recv, 1)
    proj_copy.start()

    for i in (11, 12, 13):
        loads[i].start()
    loads[9].wait()
    loads[10].wait()
    top = ids.shape[0]
    slot_row = lax.broadcasted_iota(jnp.int32, (slots, seqs), 0)
    slot_expert = slot_row // cap
    slot_rank = slot_row - slot_expert * cap
    id_rows = ids[...]
    raw = jnp.exp(logits[...])
    probs = raw / jnp.sum(raw, axis=0, keepdims=True)
    hot = jnp.zeros((slots, seqs), F32)
    prob_hot = jnp.zeros((slots, seqs), F32)
    for k in range(top):
        match = id_rows[k : k + 1, :] == slot_expert
        hot = hot + jnp.where(match, 1.0, 0.0)
        prob_hot = prob_hot + jnp.where(match, probs[k : k + 1, :], 0.0)
    earlier = (
        lax.broadcasted_iota(jnp.int32, (seqs, seqs), 0)
        < lax.broadcasted_iota(jnp.int32, (seqs, seqs), 1)
    )
    rank = dot(hot.astype(BF16), jnp.where(earlier, 1.0, 0.0).astype(BF16))
    chosen = (hot > 0.5) & (jnp.abs(rank - slot_rank.astype(F32)) < 0.5)
    placing = jnp.where(chosen, 1.0, 0.0).astype(BF16)
    weight = jnp.where(chosen, prob_hot, 0.0)
    weight_hi = weight.astype(BF16)
    weight_lo = (weight - weight_hi.astype(F32)).astype(BF16)
    group = plane * cap
    for q in range(planes):
        at = slice(q * group, (q + 1) * group)
        tables_send[q, 0] = placing[at]
        tables_send[q, 1] = weight_hi[at]
        tables_send[q, 2] = weight_lo[at]

    groups = qc // HEAD
    bias = jnp.zeros((groups, 1), F32)
    head_row = lax.broadcasted_iota(jnp.int32, (groups, 1), 0)
    for h in range(groups):
        bias = bias + jnp.where(head_row == h, bias_ref[h], 0.0)

    own_q = jnp.where(first, pq[:, :qc], pq[:, qc:])
    own_k = jnp.where(first, pk[:, :kcols], pk[:, kcols:])
    own_v = jnp.where(first, pv[:, :kcols], pv[:, kcols:])
    proj_copy.wait()
    query = (own_q + proj_recv[:, :qc]).astype(BF16).astype(F32)
    nk_ref[...] = (own_k + proj_recv[:, qc : qc + kcols]).astype(BF16)
    nv_ref[...] = (own_v + proj_recv[:, qc + kcols :]).astype(BF16)
    for h in range(groups):
        q_rows[:, h, :] = query[:, h * HEAD : (h + 1) * HEAD]

    def to_column(src, dst, sends, recvs, i):
        to = lax.rem(level + i, planes)
        return pltpu.make_async_remote_copy(
            src_ref=src.at[to],
            dst_ref=dst.at[level],
            send_sem=sends.at[i],
            recv_sem=recvs.at[i],
            device_id=(column(i), tp),
            device_id_type=MESH,
        )

    def from_column(src, dst, sends, recvs, i):
        source = lax.rem(level + planes - i, planes)
        return pltpu.make_async_remote_copy(
            src_ref=src.at[source],
            dst_ref=dst.at[source],
            send_sem=sends.at[i],
            recv_sem=recvs.at[i],
            device_id=(source * plane + spot, tp),
            device_id_type=MESH,
        )

    table_args = (tables_send, tables_recv, table_send_sem, table_recv_sem)
    for i in range(1, planes):
        to_column(*table_args, i).start()
    tables_recv[level] = tables_send[level]

    positions = kc.shape[2]
    loads[5].wait()
    place = lax.broadcasted_iota(jnp.int32, (groups, positions), 1)

    def score_step(i, carry):
        for j in range(4):
            b = i * 4 + j
            s = dot(q_rows[b].astype(BF16), kc[b]) * HEAD ** (-0.5) + bias
            z_ref[pl.ds(pl.multiple_of(b * groups, groups), groups), :] = jnp.where(
                place < lens_ref[b], s, DEAD
            )
        return carry

    lax.fori_loop(0, seqs // 4, score_step, 0)

    after = (
        lax.broadcasted_iota(jnp.int32, (POS_BLOCK, POS_BLOCK), 0)
        > lax.broadcasted_iota(jnp.int32, (POS_BLOCK, POS_BLOCK), 1)
    )
    after = jnp.where(after, 1.0, 0.0).astype(BF16)
    row_block = 64

    def break_step(i, carry):
        rows = pl.ds(pl.multiple_of(i * row_block, row_block), row_block)
        beyond = jnp.zeros((row_block, 1), F32)
        for c in reversed(range(positions // POS_BLOCK)):
            cols = slice(c * POS_BLOCK, (c + 1) * POS_BLOCK)
            z = z_ref[rows, cols]
            tail = jnp.log1p(jnp.exp(-jnp.abs(z)))
            spent = jnp.maximum(z, 0.0) + tail
            hi = spent.astype(BF16)
            lo = (spent - hi.astype(F32)).astype(BF16)
            sums = dot(jnp.concatenate([hi, lo], axis=0), after)
            inside = sums[:row_block] + sums[row_block:]
            z_ref[rows, cols] = jnp.exp(jnp.minimum(z, 0.0) - tail - (inside + beyond))
            beyond = beyond + inside[:, :1] + spent[:, :1]
        return carry

    lax.fori_loop(0, seqs * groups // row_block, break_step, 0)

    loads[6].wait()

    def read_step(i, carry):
        rows = pl.ds(pl.multiple_of(i * 4 * groups, 4 * groups), 4 * groups)
        weights = z_ref[rows, :].astype(BF16)
        values = vc[pl.ds(i * 4, 4)].reshape(4 * HEAD, positions)
        mixed = lax.dot_general(
            weights, values, (((1,), (1,)), ((), ())), preferred_element_type=F32
        )
        for j in range(4):
            att_ref[i * 4 + j] = mixed[
                j * groups : (j + 1) * groups, j * HEAD : (j + 1) * HEAD
            ]
        return carry

    lax.fori_loop(0, seqs // 4, read_step, 0)
    attended = jnp.concatenate([att_ref[:, h, :] for h in range(groups)], axis=1).astype(BF16)

    loads[7].wait()
    part = dot(attended, wo[...]).astype(BF16)
    part_send[0] = part[:, :half]
    part_send[1] = part[:, half:]
    part_copy = peer_copy(part_send, part_recv, 2)
    part_copy.start()
    loads[8].wait()
    part_copy.wait()
    mine = x_own[...].astype(F32)
    theirs = x_peer[...].astype(F32)
    res_own = (mine + (part_send[tp].astype(F32) + part_recv[tp].astype(F32))).astype(BF16)
    res_other = (
        theirs + (part_send[other].astype(F32) + part_recv[other].astype(F32))
    ).astype(BF16)
    res_ref[...] = res_own
    mine = res_own.astype(F32)
    mean, scale = stats(mine, res_other.astype(F32))
    normed_two = ((mine - mean) * scale * g2[...]).astype(BF16)
    rows_ref[...] = normed_two

    def rows_copy(i):
        return pltpu.make_async_remote_copy(
            src_ref=rows_ref,
            dst_ref=rows_recv.at[level],
            send_sem=rows_send_sem.at[i],
            recv_sem=rows_recv_sem.at[i],
            device_id=(column(i), tp),
            device_id_type=MESH,
        )

    def rows_arrival(i):
        source = lax.rem(level + planes - i, planes)
        return pltpu.make_async_remote_copy(
            src_ref=rows_ref,
            dst_ref=rows_recv.at[source],
            send_sem=rows_send_sem.at[i],
            recv_sem=rows_recv_sem.at[i],
            device_id=(source * plane + spot, tp),
            device_id_type=MESH,
        )

    def beside_copy(src, dst, sends, recvs, i, j):
        source = lax.rem(level + planes - i, planes)
        to = lax.rem(spot + j, plane)
        return pltpu.make_async_remote_copy(
            src_ref=src.at[source, to],
            dst_ref=dst.at[source, spot],
            send_sem=sends.at[i, j],
            recv_sem=recvs.at[i, j],
            device_id=(level * plane + to, tp),
            device_id_type=MESH,
        )

    def beside_arrival(src, dst, sends, recvs, i, j):
        source = lax.rem(level + planes - i, planes)
        giver = lax.rem(spot + plane - j, plane)
        return pltpu.make_async_remote_copy(
            src_ref=src.at[source, giver],
            dst_ref=dst.at[source, giver],
            send_sem=sends.at[i, j],
            recv_sem=recvs.at[i, j],
            device_id=(level * plane + giver, tp),
            device_id_type=MESH,
        )

    def fwd_copy(i, j):
        source = lax.rem(level + planes - i, planes)
        giver = lax.rem(spot + plane - j, plane)
        return pltpu.make_async_remote_copy(
            src_ref=recv_own.at[source, giver],
            dst_ref=recv_peer.at[source, giver],
            send_sem=fwd_send_sem.at[i, j],
            recv_sem=fwd_recv_sem.at[i, j],
            device_id=(ep, other),
            device_id_type=MESH,
        )

    disp_args = (disp, recv_own, disp_send_sem, disp_recv_sem)
    for i in range(1, planes):
        rows_copy(i).start()
    for i in range(1, planes):
        from_column(*table_args, i).wait_recv()
    keeps = []

    def place_rows(i, rows):
        source = lax.rem(level + planes - i, planes)
        placed = dot(tables_recv[source, 0], rows).astype(BF16)
        disp[source] = placed.reshape(plane, cap, half)
        for j in range(1, plane):
            beside_copy(*disp_args, i, j).start()
        keep = pltpu.make_async_copy(
            disp.at[source, spot], recv_own.at[source, spot], local_sem.at[i]
        )
        keep.start()
        keeps.append(keep)

    place_rows(0, normed_two)
    for i in range(1, planes):
        rows_arrival(i).wait_recv()
        place_rows(i, rows_recv[lax.rem(level + planes - i, planes)])
    for i in range(planes):
        keeps[i].wait()
        fwd_copy(i, 0).start()
        for j in range(1, plane):
            beside_arrival(*disp_args, i, j).wait_recv()
            fwd_copy(i, j).start()

    loads[11].wait()
    loads[12].wait()
    rows_block = min(slots, 256)
    row_blocks = slots // rows_block
    per_block = rows_block // group
    hidden = gate.shape[1]

    def first_half(i, carry):
        cols = pl.ds(pl.multiple_of(i * COL_BLOCK, COL_BLOCK), COL_BLOCK)
        depth = pl.ds(pl.multiple_of(tp * half, half), half)
        for r in range(row_blocks):
            rows = recv_own[r * per_block : (r + 1) * per_block].reshape(rows_block, half)
            at = slice(r * rows_block, (r + 1) * rows_block)
            gate_acc[at, cols] = dot(rows, gate[depth, cols])
            up_acc[at, cols] = dot(rows, up[depth, cols])
        return carry

    lax.fori_loop(0, hidden // COL_BLOCK, first_half, 0)

    for i in range(planes):
        for j in range(plane):
            fwd_copy(i, j).wait()

    def second_half(i, carry):
        cols = pl.ds(pl.multiple_of(i * COL_BLOCK, COL_BLOCK), COL_BLOCK)
        depth = pl.ds(pl.multiple_of(other * half, half), half)
        for r in range(row_blocks):
            rows = recv_peer[r * per_block : (r + 1) * per_block].reshape(rows_block, half)
            at = slice(r * rows_block, (r + 1) * rows_block)
            g = gate_acc[at, cols] + dot(rows, gate[depth, cols])
            u = up_acc[at, cols] + dot(rows, up[depth, cols])
            c = jnp.minimum(g, SWIGLU_LIMIT)
            linear = jnp.clip(u, -SWIGLU_LIMIT, SWIGLU_LIMIT)
            act_ref[at, cols] = (
                c * jax.nn.sigmoid(SWIGLU_ALPHA * c) * (linear + 1.0)
            ).astype(BF16)
        return carry

    lax.fori_loop(0, hidden // COL_BLOCK, second_half, 0)

    loads[13].wait()
    tiles = half // COL_BLOCK

    def down_copy(i):
        return pltpu.make_async_remote_copy(
            src_ref=down_send.at[i],
            dst_ref=down_recv.at[i],
            send_sem=down_send_sem.at[i],
            recv_sem=down_recv_sem.at[i],
            device_id=(ep, other),
            device_id_type=MESH,
        )

    def down_tile(ref, side, i):
        cols = pl.ds(pl.multiple_of(side * half + i * COL_BLOCK, COL_BLOCK), COL_BLOCK)
        for r in range(row_blocks):
            at = slice(r * rows_block, (r + 1) * rows_block)
            ref[i, at, :] = dot(act_ref[at, :], down[:, cols]).astype(BF16)

    def down_other(i, carry):
        down_tile(down_send, other, i)
        down_copy(i).start()
        return carry

    lax.fori_loop(0, tiles, down_other, 0)

    def down_mine(i, carry):
        down_tile(down_own, tp, i)
        return carry

    lax.fori_loop(0, tiles, down_mine, 0)
    for i in range(tiles):
        down_copy(i).wait()
        total = (down_own[i].astype(F32) + down_recv[i].astype(F32)).astype(BF16)
        back_send[:, :, :, i * COL_BLOCK : (i + 1) * COL_BLOCK] = total.reshape(
            planes, plane, cap, COL_BLOCK
        )

    back_args = (back_send, back_recv, back_send_sem, back_recv_sem)
    order = tuple(range(1, planes)) + (0,)
    back_keeps = {}
    for i in order:
        for j in range(1, plane):
            beside_copy(*back_args, i, j).start()
        source = lax.rem(level + planes - i, planes)
        back_keeps[i] = pltpu.make_async_copy(
            back_send.at[source, spot], back_recv.at[source, spot], local_sem.at[planes + i]
        )
        back_keeps[i].start()

    def sum_copy(i):
        source = lax.rem(level + planes - i, planes)
        return pltpu.make_async_remote_copy(
            src_ref=sum_send.at[source],
            dst_ref=sum_recv.at[level],
            send_sem=sum_send_sem.at[i],
            recv_sem=sum_recv_sem.at[i],
            device_id=(source * plane + spot, tp),
            device_id_type=MESH,
        )

    def sum_arrival(i):
        giver = lax.rem(level + i, planes)
        return pltpu.make_async_remote_copy(
            src_ref=sum_send.at[giver],
            dst_ref=sum_recv.at[giver],
            send_sem=sum_send_sem.at[i],
            recv_sem=sum_recv_sem.at[i],
            device_id=(giver * plane + spot, tp),
            device_id_type=MESH,
        )

    over_slots = (((0,), (0,)), ((), ()))
    total = res_ref[...].astype(F32)
    for i in order:
        source = lax.rem(level + planes - i, planes)
        back_keeps[i].wait()
        for j in range(1, plane):
            beside_arrival(*back_args, i, j).wait_recv()
        back = back_recv[source].reshape(group, half)
        mixed = lax.dot_general(
            tables_recv[source, 1], back, over_slots, preferred_element_type=F32
        ) + lax.dot_general(tables_recv[source, 2], back, over_slots, preferred_element_type=F32)
        if i == 0:
            total = total + mixed
        else:
            sum_send[source] = mixed.astype(BF16)
            sum_copy(i).start()
    for i in range(1, planes):
        sum_arrival(i).wait_recv()
        total = total + sum_recv[lax.rem(level + i, planes)].astype(F32)
    out_ref[...] = total.astype(BF16)

    for i in range(1, planes):
        to_column(*table_args, i).wait_send()
        rows_copy(i).wait_send()
        sum_copy(i).wait_send()
    for i in range(planes):
        for j in range(1, plane):
            beside_copy(*disp_args, i, j).wait_send()
            beside_copy(*back_args, i, j).wait_send()


def local(
    tokens,
    norm1_gain,
    w_query,
    w_key,
    w_value,
    head_bias,
    key_cache,
    value_cache,
    seq_lengths,
    w_out,
    norm2_gain,
    route_ids,
    route_logits,
    expert_gate,
    expert_up,
    expert_down,
):
    n = lax.axis_size("ep")
    seqs, half = tokens.shape
    top = route_ids.shape[1]
    experts = n * expert_gate.shape[0]
    capacity = max(2, 2 * seqs * top // experts)
    cap = -(-capacity // 16) * 16
    slots = n * cap
    planes = 4 if n % 4 == 0 else 1
    plane = n // planes
    qc = w_query.shape[1] // 2
    kcols = w_key.shape[1] // 2
    groups = qc // HEAD
    positions = key_cache.shape[1]
    hidden = expert_gate.shape[2]
    tiles = half // COL_BLOCK
    keys = jnp.swapaxes(key_cache, 1, 2)
    values = jnp.swapaxes(value_cache, 1, 2)
    operands = (
        tokens,
        norm1_gain.reshape(1, -1),
        w_query,
        w_key,
        w_value,
        head_bias,
        keys,
        values,
        seq_lengths,
        w_out,
        norm2_gain.reshape(1, -1),
        route_ids.T,
        route_logits.T,
        expert_gate.reshape(expert_gate.shape[1:]),
        expert_up.reshape(expert_up.shape[1:]),
        expert_down.reshape(expert_down.shape[1:]),
    )
    in_smem = (5, 8)
    in_specs = [
        pl.BlockSpec(memory_space=pltpu.SMEM if i in in_smem else pl.ANY)
        for i in range(len(operands))
    ]
    vmem = pl.BlockSpec(memory_space=pltpu.VMEM)
    loaded = [
        pltpu.VMEM(a.shape, a.dtype) for i, a in enumerate(operands) if i not in in_smem
    ]
    dma = pltpu.SemaphoreType.DMA
    scratch = (
        [loaded[0], loaded[0]]
        + loaded[1:]
        + [
            pltpu.VMEM((seqs, qc + 2 * kcols), F32),
            pltpu.VMEM((seqs, qc + 2 * kcols), F32),
            pltpu.VMEM((seqs, groups, HEAD), F32),
            pltpu.VMEM((seqs * groups, positions), F32),
            pltpu.VMEM((seqs, groups, HEAD), F32),
            pltpu.VMEM((2, seqs, half), BF16),
            pltpu.VMEM((2, seqs, half), BF16),
            pltpu.VMEM((seqs, half), BF16),
            pltpu.VMEM((planes, 3, plane * cap, seqs), BF16),
            pltpu.VMEM((planes, 3, plane * cap, seqs), BF16),
            pltpu.VMEM((seqs, half), BF16),
            pltpu.VMEM((planes, seqs, half), BF16),
            pltpu.VMEM((planes, plane, cap, half), BF16),
            pltpu.VMEM((planes, plane, cap, half), BF16),
            pltpu.VMEM((planes, plane, cap, half), BF16),
            pltpu.VMEM((slots, hidden), F32),
            pltpu.VMEM((slots, hidden), F32),
            pltpu.VMEM((slots, hidden), BF16),
            pltpu.VMEM((tiles, slots, COL_BLOCK), BF16),
            pltpu.VMEM((tiles, slots, COL_BLOCK), BF16),
            pltpu.VMEM((tiles, slots, COL_BLOCK), BF16),
            pltpu.VMEM((planes, plane, cap, half), BF16),
            pltpu.VMEM((planes, plane, cap, half), BF16),
            pltpu.VMEM((planes, seqs, half), BF16),
            pltpu.VMEM((planes, seqs, half), BF16),
            dma((len(loaded),)),
            dma((3,)),
            dma((3,)),
            dma((planes,)),
            dma((planes,)),
            dma((planes,)),
            dma((planes,)),
            dma((planes,)),
            dma((planes,)),
            dma((planes, plane)),
            dma((planes, plane)),
            dma((planes, plane)),
            dma((planes, plane)),
            dma((tiles,)),
            dma((tiles,)),
            dma((planes, plane)),
            dma((planes, plane)),
            dma((2 * planes,)),
        ]
    )
    return pl.pallas_call(
        functools.partial(kernel, n, cap),
        out_shape=(
            jax.ShapeDtypeStruct((seqs, half), BF16),
            jax.ShapeDtypeStruct((seqs, kcols), BF16),
            jax.ShapeDtypeStruct((seqs, kcols), BF16),
        ),
        in_specs=in_specs,
        out_specs=(vmem, vmem, vmem),
        scratch_shapes=scratch,
        compiler_params=pltpu.CompilerParams(
            collective_id=0, has_side_effects=True, vmem_limit_bytes=64 * 1024 * 1024 - 65536
        ),
    )(*operands)


def solution(mesh):
    in_specs = (
        P("ep", "tp"),
        P("tp"),
        P("tp", None),
        P("tp", None),
        P("tp", None),
        P("tp"),
        P("ep", None, "tp"),
        P("ep", None, "tp"),
        P("ep"),
        P("tp", None),
        P("tp"),
        P("ep", None),
        P("ep", None),
        P("ep", None, "tp"),
        P("ep", None, "tp"),
        P("ep", "tp", None),
    )
    out_specs = (P("ep", "tp"), P("ep", "tp"), P("ep", "tp"))
    return jax.shard_map(local, mesh=mesh, in_specs=in_specs, out_specs=out_specs, check_vma=False)
```
